256 devices in a mesh: ep: 32 (over z, x), tp: 8 (over y, core).
Axes of the slice: x: 4, y: 4, z: 8, core: 2. Of those that a mesh axis runs over, the one named last changes fastest.
Arguments:
- resid: bfloat16 [1024, 2048], P('ep'), may hold values from -6 to 6
- norm_gain: bfloat16 [2048], replicated, may hold values from 0.099609375 to 1.8984375
- w_query: bfloat16 [2048, 1024], P(None, 'tp'), may hold values from -0.125 to 0.125
- w_key: bfloat16 [2048, 1024], P(None, 'tp'), may hold values from -0.125 to 0.125
- w_value: bfloat16 [2048, 1024], P(None, 'tp'), may hold values from -0.125 to 0.125
- w_gate: bfloat16 [2048, 1024], P(None, 'tp'), may hold values from -0.125 to 0.125
- head_gain: bfloat16 [1024], P('tp'), may hold values from 0.099609375 to 1.8984375
- w_output: bfloat16 [1024, 2048], P('tp'), may hold values from -0.1875 to 0.1875
- state: float32 [1024, 8, 128, 128], P('ep', 'tp'), may hold values from -0.6 to 0.6
- positions: int32 [1024], P('ep'), may hold values from 1024 to 8191
- ffn_gain: bfloat16 [2048], replicated, may hold values from 0.099609375 to 1.8984375
- w_mix: bfloat16 [2048], replicated, may hold values from -0.125 to 0.125
- dense_gate: bfloat16 [2048, 5632], P('tp', 'ep'), may hold values from -0.125 to 0.125
- dense_up: bfloat16 [2048, 5632], P('tp', 'ep'), may hold values from -0.125 to 0.125
- dense_down: bfloat16 [5632, 2048], P('ep', 'tp'), may hold values from -0.15625 to 0.15625
- routes: int32 [1024, 2], P('ep'), may hold values from 0 to 31, all different within a row; in each aligned block of 32 rows (0 to 31, 32 to 63, ...) at most 4 rows name the same one
- route_weight: bfloat16 [1024, 2], P('ep'), may hold values from 0.19921875 to 1
- expert_gate: bfloat16 [32, 2048, 4096], P('ep', None, 'tp'), may hold values from -0.125 to 0.125
- expert_up: bfloat16 [32, 2048, 4096], P('ep', None, 'tp'), may hold values from -0.125 to 0.125
- expert_down: bfloat16 [32, 4096, 2048], P('ep', 'tp'), may hold values from -0.09375 to 0.09375
Outputs:
- final: bfloat16 [1024, 2048], P('ep', 'tp')
- new_state: float32 [1024, 8, 128, 128], P('ep', 'tp')
The draws below stay inside these ranges and needn't reach their ends.
Inputs may be any that keep to these rules, and one draw needn't show every extreme that they name: `routes`: each row names 2 different experts; in the rows of one index of ep no expert is named by more than 4 rows, a bound that some block reaches; every expert is named by some row.
All inputs are finite; a program needn't handle non-finite values.
Results may differ from the reference program's by a relative error of at most 0.018.
Values may be sent and summed in bfloat16 or wider, within the bound.
No kernel may reach another device: no remote copies, remote signals or barrier semaphores. Data moves between devices by JAX's collectives and lax.ppermute only.
A program may use at most 64 MiB of HBM per device.

```python
import math
import jax
import jax.numpy as jnp
import numpy as np
from jax import lax

D = 2048
RET_HEADS = 8
HEAD_DIM = 128
RET_W = 1024
FFD = 5632
FFE = 4096
TOPK = 2
SEQ_DEV = 32
SEQS = 1024
EXPERTS = 32
CAP = 4
N_EP = 32
N_TP = 8


def place_ends(values, key, low, top_value):
    place = [jax.random.randint(jax.random.fold_in(key, axis), (), 0, length) for axis, length in enumerate(values.shape)]
    longest = values.shape.index(max(values.shape))
    neighbour = place[:longest] + [(place[longest] + 1) % values.shape[longest]] + place[longest + 1:]
    return values.at[tuple(place)].set(low).at[tuple(neighbour)].set(top_value)


def with_spikes(entries, own_key, source, target, parts, factor):
    def block_of(axis_at):
        return (jnp.arange(entries.shape[axis_at]) // (entries.shape[axis_at] // parts)).reshape((-1,) + (1,) * (entries.ndim - 1 - axis_at))

    near = jax.random.permutation(own_key, parts)[block_of(target)]
    far = (block_of(target) + parts // 2) % parts
    return jnp.where((block_of(source) == near) | (block_of(source) == far), factor * entries, entries)


def level_of(rng, dims, shards, low, top_value):
    factor_of = 1.0
    for dim, parts in shards:
        draws = jax.random.uniform(jax.random.fold_in(jax.random.fold_in(rng, 6), dim), (parts,), jnp.float32, low / len(shards), top_value / len(shards))
        factor_of = factor_of * jnp.repeat(jnp.exp(draws), dims[dim] // parts).reshape((-1,) + (1,) * (len(dims) - 1 - dim))
    return factor_of


def shared_out(rng, own, number, rows, count, top, bound, lean):
    sequence = jax.random.permutation(rng, count)
    heavy_load, usual = load_shares(count, rows * top, bound, lean, True), load_shares(count, rows * top, bound, lean, False)
    places = jnp.arange(count)

    def named(tallies, offset_by):
        used = int((tallies > 0).sum())
        fixed = max(1, used // 4)
        moved = fixed + (places - fixed + offset_by * (used - fixed)) % max(1, count - fixed)
        return jnp.zeros((count,), jnp.int32).at[sequence[jnp.where(places < fixed, places, moved)]].set(jnp.asarray(tallies, jnp.int32))

    tallies = jnp.where(number % 4 == 0, named(heavy_load, number // 4), named(usual, number - number // 4 - 1))
    mixed = jax.random.permutation(jax.random.fold_in(own, 3), count)
    source_of, receiver = mixed[0:count // 2 * 2:2], mixed[1:count // 2 * 2:2]
    margin = jnp.minimum(tallies[source_of] - 1, bound - tallies[receiver]) // 2
    margin = jnp.where((source_of == sequence[0]) | (receiver == sequence[0]) | (tallies[receiver] == 0), 0, jnp.maximum(margin, 0))
    moved = jax.random.randint(jax.random.fold_in(own, 4), (count // 2,), 0, 1 << 20) % (margin + 1)
    tallies = tallies.at[source_of].add(-moved).at[receiver].add(moved)
    labels = jnp.searchsorted(jnp.cumsum(tallies), jnp.arange(rows * top), side="right").astype(jnp.int32)
    grid = labels.reshape(top, rows).T
    grid = grid[jax.random.permutation(jax.random.fold_in(own, 1), rows)]
    offset_by = jax.random.randint(jax.random.fold_in(own, 2), (rows, 1), 0, top)
    return jnp.take_along_axis(grid, (jnp.arange(top)[None, :] + offset_by) % top, axis=1)


def load_shares(number_of, total, limit, skew, full):
    portions = [(1 << 20) // math.isqrt(rank ** skew) + 1 for rank in range(1, number_of + 1)]
    largest = limit if full else min(limit, max(-(-total // number_of), total * portions[0] // sum(portions)))
    least = 1 if total - largest >= number_of - 1 else 0
    given, rest = [largest] + [least] * (number_of - 1), total - largest - least * (number_of - 1)
    while rest > 0:
        free = [i for i in range(1, number_of) if given[i] < largest] or [i for i in range(1, number_of) if given[i] < limit]
        mass, remaining = sum([portions[i] for i in free]), rest
        for i in free:
            extra = min(limit - given[i], max(1, remaining * portions[i] // mass), rest)
            given[i] = given[i] + extra
            rest = rest - extra
    return np.array(given)


def scatter_about(stream_key, dims, deviation, limit, cuts=(), held_as=jnp.bfloat16):
    values = jax.random.normal(stream_key, dims, jnp.float32) * deviation
    if len(cuts) > 0:
        values = level_of(stream_key, dims, cuts, -0.22, 0.18) * values
    return jnp.clip(values, min=-limit, max=limit).astype(held_as)


def heavy_noise(own_key, dims, scale, most, cuts, heavy, kind=jnp.bfloat16):
    values = scale * jax.random.normal(own_key, dims, jnp.float32)
    if cuts:
        values = values * level_of(own_key, dims, cuts, -0.22, 0.18)
    return jnp.clip(with_spikes(values, jax.random.fold_in(own_key, 3), *heavy), -most, most).astype(kind)


def setup_inputs(seed: int = 0) -> dict:
    splits = jax.random.split(jax.random.key(seed), 21)
    resid = scatter_about(splits[0], (SEQS, D), 1.0, 6.0, ((0, 32),))
    norm_gain = jnp.clip(1.0 + 0.18 * jax.random.normal(splits[1], (D,), jnp.float32), 0.099609375, 1.8984375).astype(jnp.bfloat16)
    w_query = scatter_about(splits[2], (D, RET_W), D ** -0.5, 0.125, ((1, 8),))
    w_key = scatter_about(splits[3], (D, RET_W), D ** -0.5, 0.125, ((1, 8),))
    w_value = scatter_about(splits[4], (D, RET_W), D ** -0.5, 0.125, ((1, 8),))
    w_gate = scatter_about(splits[5], (D, RET_W), D ** -0.5, 0.125, ((1, 8),))
    head_gain = jnp.clip(1.0 + 0.18 * jax.random.normal(splits[6], (RET_W,), jnp.float32), 0.099609375, 1.8984375).astype(jnp.bfloat16)
    w_output = scatter_about(splits[7], (RET_W, D), RET_W ** -0.5, 0.1875, ((0, 8),))
    state = scatter_about(splits[8], (SEQS, RET_HEADS, HEAD_DIM, HEAD_DIM), 0.1, 0.6, ((0, 32), (1, 8)), jnp.float32)
    positions = place_ends(jax.random.randint(splits[9], (SEQS,), 1024, 8192), jax.random.fold_in(splits[9], 1), 1024, 8191).astype(jnp.int32)
    ffn_gain = jnp.clip(1.0 + 0.18 * jax.random.normal(splits[10], (D,), jnp.float32), 0.099609375, 1.8984375).astype(jnp.bfloat16)
    w_mix = scatter_about(splits[11], (D,), D ** -0.5, 0.125)
    dense_gate = scatter_about(splits[12], (D, FFD), D ** -0.5, 0.125, ((0, 8), (1, 32)))
    dense_up = scatter_about(splits[13], (D, FFD), D ** -0.5, 0.125, ((0, 8), (1, 32)))
    dense_down = heavy_noise(splits[14], (FFD, D), FFD ** -0.5, 0.15625, ((0, 32), (1, 8)), (0, 1, 32, 2.75))
    routes_keys = jax.random.split(jax.random.fold_in(splits[15], 1), SEQS // SEQ_DEV)
    routes_turns = jax.random.permutation(jax.random.fold_in(splits[15], 3), SEQS // SEQ_DEV)
    routes = jax.vmap(lambda own, number: shared_out(jax.random.fold_in(splits[15], 2), own, number, SEQ_DEV, EXPERTS, TOPK, CAP, 2))(routes_keys, routes_turns).reshape((SEQS, TOPK))
    route_weight = jnp.clip(0.19921875 + 0.80078125 * jax.random.uniform(splits[16], (SEQS, TOPK), jnp.float32) ** level_of(splits[16], (SEQS, TOPK), ((0, 32),), -0.2, 0.2), 0.19921875, 1.0).astype(jnp.bfloat16)
    expert_gate = scatter_about(splits[17], (EXPERTS, D, FFE), D ** -0.5, 0.125, ((0, 32), (2, 8)))
    expert_up = scatter_about(splits[18], (EXPERTS, D, FFE), D ** -0.5, 0.125, ((0, 32), (2, 8)))
    expert_down = scatter_about(splits[19], (EXPERTS, FFE, D), FFE ** -0.5, 0.09375, ((0, 32), (1, 8)))
    return dict(resid=resid, norm_gain=norm_gain, w_query=w_query, w_key=w_key, w_value=w_value, w_gate=w_gate, head_gain=head_gain, w_output=w_output, state=state, positions=positions, ffn_gain=ffn_gain, w_mix=w_mix, dense_gate=dense_gate, dense_up=dense_up, dense_down=dense_down, routes=routes, route_weight=route_weight, expert_gate=expert_gate, expert_up=expert_up, expert_down=expert_down)


EPSILON = 1e-06
THETA = 10000.0

def rms_norm(inputs, scaling):
    square = lax.optimization_barrier(jnp.mean(inputs * inputs, axis=-1, keepdims=True))
    return inputs * lax.rsqrt(square + EPSILON) * scaling.astype(jnp.float32)

def rounded(partial_value):
    return lax.optimization_barrier(partial_value.astype(jnp.bfloat16)).astype(jnp.float32)

def rotate(inputs, places):
    halfway = inputs.shape[-1] // 2
    inverse = THETA ** (-jnp.arange(halfway, dtype=jnp.float32) / halfway)
    angles = places.astype(jnp.float32)[:, None] * inverse[None, :]
    cosine = jnp.cos(angles)[:, None, :]
    sine_of = jnp.sin(angles)[:, None, :]
    former = inputs[..., :halfway]
    latter = inputs[..., halfway:]
    return jnp.concatenate([former * cosine - latter * sine_of, former * sine_of + latter * cosine], axis=-1)

def retain(queries, keys_in, values_in, gating, memory, places, head_first, head_gain):
    seqs_here = queries.shape[0]
    heads_here = memory.shape[1]
    head_size = memory.shape[2]
    head_shape = (seqs_here, heads_here, head_size)
    query_rot = rotate(queries.astype(jnp.float32).reshape(head_shape), places)
    key_rot = rotate(keys_in.astype(jnp.float32).reshape(head_shape), places) * head_size ** (-0.5)
    value_heads = values_in.astype(jnp.float32).reshape(head_shape)
    head_index = head_first + jnp.arange(heads_here, dtype=jnp.float32)
    decays = 1.0 - jnp.exp2(-1.0 - 1.5 * head_index)
    within = lax.optimization_barrier(jnp.sum(query_rot * key_rot, axis=-1, keepdims=True)) * value_heads
    carried = jnp.einsum('shd,shde->she', query_rot, memory, precision=lax.Precision.HIGHEST) * decays[None, :, None]
    mixture = within + carried
    new_memory = decays[None, :, None, None] * memory + key_rot[:, :, :, None] * value_heads[:, :, None, :]
    centre = lax.optimization_barrier(jnp.mean(mixture, axis=-1, keepdims=True))
    spread = lax.optimization_barrier(jnp.mean(jnp.square(mixture - centre), axis=-1, keepdims=True))
    normed = ((mixture - centre) * lax.rsqrt(spread + EPSILON)).reshape(seqs_here, heads_here * head_size)
    normed = normed * head_gain.astype(jnp.float32)
    output = (jax.nn.silu(gating.astype(jnp.float32)) * normed).astype(jnp.bfloat16)
    return (output, new_memory)

def select_slots(route_ids, expert, max_rows):
    flat_ids = route_ids.reshape(-1)
    hits = (flat_ids == expert).astype(jnp.int32)
    ranks = jnp.cumsum(hits) - 1
    slot_range = jnp.arange(max_rows, dtype=jnp.int32)
    matches = (hits[None, :] == 1) & (ranks[None, :] == slot_range[:, None])
    flat_index = jnp.arange(flat_ids.shape[0], dtype=jnp.int32)
    picked = lax.optimization_barrier(jnp.sum(jnp.where(matches, flat_index[None, :], 0), axis=1)).astype(jnp.int32)
    filled = jnp.any(matches, axis=1)
    return (picked, filled)

def expert_hidden(chosen, gate_weight, up_weight):
    gate_value = jnp.dot(chosen, gate_weight, preferred_element_type=jnp.float32)
    up_value = jnp.dot(chosen, up_weight, preferred_element_type=jnp.float32)
    return (jax.nn.silu(gate_value) * up_value).astype(jnp.bfloat16)

def reference(resid, norm_gain, w_query, w_key, w_value, w_gate, head_gain, w_output, state, positions, ffn_gain, w_mix, dense_gate, dense_up, dense_down, routes, route_weight, expert_gate, expert_up, expert_down):
    normed_in = rms_norm(resid.astype(jnp.float32), norm_gain).astype(jnp.bfloat16)

    def project(weight):
        return jnp.dot(normed_in, weight, preferred_element_type=jnp.float32).astype(jnp.bfloat16)
    retained, new_state = retain(project(w_query), project(w_key), project(w_value), project(w_gate), state, positions, 0.0, head_gain)
    width_tp = w_output.shape[0] // N_TP
    attention = jnp.zeros(resid.shape, jnp.float32)
    for block in range(N_TP):
        lower = block * width_tp
        attention = attention + rounded(jnp.dot(retained[:, lower:lower + width_tp], w_output[lower:lower + width_tp], preferred_element_type=jnp.float32))
    middle = resid.astype(jnp.float32) + attention
    normed_mid = rms_norm(middle, ffn_gain).astype(jnp.bfloat16)
    mixing = jax.nn.sigmoid(jnp.dot(normed_mid, w_mix[:, None], preferred_element_type=jnp.float32))
    model_tp = D // N_TP
    gate_sum = jnp.zeros((resid.shape[0], FFD), jnp.float32)
    up_sum = jnp.zeros((resid.shape[0], FFD), jnp.float32)
    for block in range(N_TP):
        lower = block * model_tp
        columns = normed_mid[:, lower:lower + model_tp]
        gate_sum = gate_sum + rounded(jnp.dot(columns, dense_gate[lower:lower + model_tp], preferred_element_type=jnp.float32))
        up_sum = up_sum + rounded(jnp.dot(columns, dense_up[lower:lower + model_tp], preferred_element_type=jnp.float32))
    dense_hidden = (jax.nn.silu(gate_sum) * up_sum).astype(jnp.bfloat16)
    hidden_ep = FFD // N_EP

    def dense_block(total, block):
        lower = block * hidden_ep
        part_hidden = lax.dynamic_slice_in_dim(dense_hidden, lower, hidden_ep, 1)
        part_down = lax.dynamic_slice_in_dim(dense_down, lower, hidden_ep, 0)
        return (total + rounded(jnp.dot(part_hidden, part_down, preferred_element_type=jnp.float32)), None)
    dense_out, _ = lax.scan(dense_block, jnp.zeros(resid.shape, jnp.float32), jnp.arange(N_EP, dtype=jnp.int32))
    max_rows = N_EP * CAP
    expert_tp = FFE // N_TP
    flat_weight = route_weight.reshape(-1).astype(jnp.float32)

    def one_expert(total, expert):
        picked, filled = select_slots(routes, expert, max_rows)
        token_rows = picked // TOPK
        chosen = normed_mid[token_rows]
        hidden_e = expert_hidden(chosen, expert_gate[expert], expert_up[expert])
        summed = jnp.zeros((max_rows, D), jnp.float32)
        for block in range(N_TP):
            lower = block * expert_tp
            summed = summed + rounded(jnp.dot(hidden_e[:, lower:lower + expert_tp], expert_down[expert, lower:lower + expert_tp], preferred_element_type=jnp.float32))
        result = rounded(summed)
        weights_e = jnp.where(filled, flat_weight[picked], 0.0)
        total = total.at[token_rows].add(weights_e[:, None] * result)
        return (total, None)
    moe_out, _ = lax.scan(one_expert, jnp.zeros(resid.shape, jnp.float32), jnp.arange(EXPERTS, dtype=jnp.int32))
    final = (middle + moe_out + mixing * dense_out).astype(jnp.bfloat16)
    return (final, new_state)
```

```python
import jax
import jax.numpy as jnp
from jax import lax
from jax.sharding import Mesh, PartitionSpec as P

EPSILON = 1e-06
THETA = 10000.0
EP = ("z", "x")
TP = ("y", "c")
BF = jnp.bfloat16
F32 = jnp.float32


def exchange(value, axis):
    return lax.all_to_all(value, axis, split_axis=0, concat_axis=0, tiled=True)


def swap_cores(value):
    return lax.ppermute(value, "c", [(0, 1), (1, 0)])


def dot(a, b):
    return jnp.dot(a, b, preferred_element_type=F32)


def dot_nt(a, b):
    return lax.dot_general(a, b, (((1,), (1,)), ((), ())), preferred_element_type=F32)


def dot_tn(a, b):
    return lax.dot_general(a, b, (((0,), (0,)), ((), ())), preferred_element_type=F32)


def rms_norm(inputs, scaling):
    square = jnp.mean(inputs * inputs, axis=-1, keepdims=True)
    return inputs * lax.rsqrt(square + EPSILON) * scaling.astype(F32)


def rotate(inputs, places):
    halfway = inputs.shape[-1] // 2
    inverse = THETA ** (-jnp.arange(halfway, dtype=F32) / halfway)
    angles = places.astype(F32)[:, None] * inverse[None, :]
    cosine = jnp.cos(angles)[:, None, :]
    sine_of = jnp.sin(angles)[:, None, :]
    former = inputs[..., :halfway]
    latter = inputs[..., halfway:]
    return jnp.concatenate(
        [former * cosine - latter * sine_of, former * sine_of + latter * cosine], axis=-1
    )


def retain(queries, keys_in, values_in, gating, memory, places, head_first, head_gain):
    seqs_here = queries.shape[0]
    heads_here = memory.shape[1]
    head_size = memory.shape[2]
    head_shape = (seqs_here, heads_here, head_size)
    query_rot = rotate(queries.astype(F32).reshape(head_shape), places)
    key_rot = rotate(keys_in.astype(F32).reshape(head_shape), places) * head_size ** (-0.5)
    value_heads = values_in.astype(F32).reshape(head_shape)
    head_index = head_first + jnp.arange(heads_here, dtype=F32)
    decays = 1.0 - jnp.exp2(-1.0 - 1.5 * head_index)
    within = jnp.sum(query_rot * key_rot, axis=-1, keepdims=True) * value_heads
    carried = jnp.einsum("shd,shde->she", query_rot, memory) * decays[None, :, None]
    mixture = within + carried
    new_memory = (
        decays[None, :, None, None] * memory + key_rot[:, :, :, None] * value_heads[:, :, None, :]
    )
    centre = jnp.mean(mixture, axis=-1, keepdims=True)
    spread = jnp.mean(jnp.square(mixture - centre), axis=-1, keepdims=True)
    normed = ((mixture - centre) * lax.rsqrt(spread + EPSILON)).reshape(
        seqs_here, heads_here * head_size
    )
    normed = normed * head_gain.astype(F32)
    output = (jax.nn.silu(gating.astype(F32)) * normed).astype(BF)
    return (output, new_memory)


def row_places(routes, experts):
    ids = jnp.arange(experts, dtype=jnp.int32)
    named = jnp.any(routes[:, :, None] == ids[None, None, :], axis=1).astype(jnp.int32)
    before = jnp.cumsum(named, axis=0) - named
    total = jnp.sum(named, axis=0, keepdims=True)
    earlier = jnp.arange(routes.shape[0], dtype=jnp.int32)[:, None]
    return jnp.where(named == 1, before, total + earlier - before)


def per_device(
    resid, norm_gain, w_query, w_key, w_value, w_gate, head_gain, w_output, state, positions,
    ffn_gain, w_mix, dense_gate, dense_up, dense_down, routes, route_weight,
    expert_gate, expert_up, expert_down,
):
    seqs, width = resid.shape
    n_y, n_c = lax.axis_size("y"), lax.axis_size("c")
    n_tp = n_y * n_c
    n_ep = lax.axis_size("z") * lax.axis_size("x")
    cols = width // n_tp
    core = lax.axis_index("c")
    tp = lax.axis_index("y") * n_c + core
    slots = max(2, 2 * seqs * routes.shape[1] // n_ep)
    hid = dense_gate.shape[1]

    own_w = jnp.concatenate([dense_gate.T, dense_up.T], axis=0)
    pair_w = jnp.concatenate([own_w, swap_cores(own_w)], axis=1)

    normed_in = rms_norm(resid.astype(F32), norm_gain).astype(BF)

    def project(weight):
        return dot(normed_in, weight).astype(BF)

    heads_here = state.shape[1]
    retained, new_state = retain(
        project(w_query), project(w_key), project(w_value), project(w_gate),
        state, positions, (tp * heads_here).astype(F32), head_gain,
    )
    partial = dot(retained, w_output).astype(BF)
    partial = jnp.moveaxis(partial.reshape(seqs, n_tp, cols), 1, 0)
    arrived = exchange(partial, TP)

    def own_columns(matrix, block):
        return lax.dynamic_slice_in_dim(matrix, block * cols, cols, matrix.ndim - 1)

    middle = own_columns(resid, tp).astype(F32) + jnp.sum(arrived.astype(F32), axis=0)
    middle_cut = middle.astype(BF)

    place = row_places(routes, n_ep)
    sorting = (place.T[:, None, :] == jnp.arange(seqs, dtype=jnp.int32)[None, :, None]).astype(BF)
    sorting = sorting.reshape(n_ep * seqs, seqs)
    outgoing = dot(sorting, middle_cut).astype(BF).reshape(n_ep, seqs, cols)
    rows = exchange(outgoing, EP)

    chosen = rows[:, :slots].reshape(n_ep * slots, cols)
    chosen_other = swap_cores(chosen)
    flat = rows.reshape(n_ep * seqs, cols)
    half = n_ep * seqs // n_c
    kept = lax.dynamic_slice_in_dim(flat, core * half, half, 0)
    gained = swap_cores(lax.dynamic_slice_in_dim(flat, (1 - core) * half, half, 0))
    both = jnp.concatenate([kept, gained], axis=1).astype(F32)
    gains = jnp.concatenate([own_columns(ffn_gain, tp), own_columns(ffn_gain, tp ^ 1)])
    mixers = jnp.concatenate([own_columns(w_mix, tp), own_columns(w_mix, tp ^ 1)])
    scaled = (both * gains.astype(F32)).astype(BF)
    weights = jnp.concatenate([pair_w, mixers[None, :], jnp.zeros((7, n_c * cols), BF)], axis=0)
    sums = dot_nt(weights, scaled)
    squares = dot_nt(jnp.ones((8, n_c * cols), BF), (both * both).astype(BF))
    lower = jnp.concatenate([sums[2 * hid : 2 * hid + 1], squares[:7]], axis=0)
    sums = jnp.concatenate([sums[: 2 * hid], lower], axis=0).astype(BF)
    part = half // n_y
    sums = jnp.moveaxis(sums.reshape(2 * hid + 8, n_y, part), 1, 0)
    ordered = jnp.where(core == 0, jnp.concatenate([chosen, chosen_other], axis=1),
                        jnp.concatenate([chosen_other, chosen], axis=1))
    n_slots = n_ep * slots
    pieces = jnp.moveaxis(ordered.reshape(n_slots, n_c * cols // part, part), 1, 0)
    pieces = pieces.reshape(1, -1, part)
    sent = jnp.concatenate([sums, jnp.broadcast_to(pieces, (n_y, *pieces.shape[1:]))], axis=1)
    got = exchange(sent, "y")

    sums = jnp.sum(got[:, : 2 * hid + 8].astype(F32), axis=0)
    scale = lax.rsqrt(sums[2 * hid + 1 : 2 * hid + 2] / width + EPSILON)
    mixing = jax.nn.sigmoid(sums[2 * hid : 2 * hid + 1] * scale)
    dense_hidden = jax.nn.silu(sums[:hid] * scale) * (sums[hid : 2 * hid] * scale) * mixing
    dense_hidden = dense_hidden.astype(BF)
    hidden_pair = swap_cores(dense_hidden)

    pieces = got[:, 2 * hid + 8 :].reshape(n_y * n_c * cols // part, n_slots, part)
    chosen = jnp.moveaxis(pieces, 0, 1).reshape(n_slots, width).astype(F32)
    chosen = rms_norm(chosen, ffn_gain).astype(BF)
    hidden = jax.nn.silu(dot(chosen, expert_gate[0])) * dot(chosen, expert_up[0])
    down = dot(hidden.astype(BF), expert_down[0]).astype(BF)
    down = jnp.moveaxis(down.reshape(n_slots, n_y, n_c, cols), 2, 0)
    down_kept = lax.dynamic_index_in_dim(down, core, 0, False)
    down_got = swap_cores(lax.dynamic_index_in_dim(down, 1 - core, 0, False))
    down = (down_kept.astype(F32) + down_got.astype(F32)).astype(BF)
    down = jnp.moveaxis(down.reshape(n_slots, n_y, cols // part, part), 0, 2)
    down = down.reshape(n_y, cols // part * n_slots, part)
    hiddens = jnp.where(core == 0, jnp.concatenate([dense_hidden, hidden_pair], axis=0),
                        jnp.concatenate([hidden_pair, dense_hidden], axis=0))
    sent = jnp.concatenate([down, jnp.broadcast_to(hiddens[None], (n_y, *hiddens.shape))], axis=1)
    got = exchange(sent, "y")

    at = cols // part * n_slots
    result = jnp.sum(got[:, :at].astype(F32), axis=0).astype(BF)
    result = result.reshape(cols // part, n_ep, slots, part)
    hiddens = got[:, at:].reshape(n_y, n_c, hid, part)
    hiddens = jnp.moveaxis(hiddens, 2, 0)
    hiddens = jnp.moveaxis(hiddens, 2, 1).reshape(hid, n_ep * seqs)
    dense_back = dot_tn(hiddens, dense_down).astype(BF).reshape(n_ep, seqs, cols)
    back = jnp.concatenate(
        [dense_back[:, :, i * part : (i + 1) * part] for i in range(cols // part)]
        + [result[i] for i in range(cols // part)], axis=1,
    )
    back = exchange(back, EP)

    ids = jnp.arange(n_ep, dtype=jnp.int32)
    slot_ids = jnp.arange(slots, dtype=jnp.int32)
    weight_of = jnp.sum(
        jnp.where(routes[:, :, None] == ids, route_weight.astype(F32)[:, :, None], 0.0), axis=1
    )
    weighing = jnp.where(place[:, :, None] == slot_ids, weight_of[:, :, None], 0.0).astype(BF)
    weighing = weighing.reshape(seqs, n_slots)
    total = []
    for i in range(cols // part):
        dense_rows = back[:, i * seqs : (i + 1) * seqs].reshape(n_ep * seqs, part)
        first = cols // part * seqs + i * slots
        expert_rows = back[:, first : first + slots].reshape(n_slots, part)
        total.append(dot_tn(sorting, dense_rows) + dot(weighing, expert_rows))
    final = (middle + jnp.concatenate(total, axis=1)).astype(BF)
    return (final, new_state)


def solution(mesh):
    inner = Mesh(mesh.devices.reshape(8, 4, 4, 2), ("z", "x", "y", "c"))
    in_specs = (
        P(EP, None), P(), P(None, TP), P(None, TP), P(None, TP), P(None, TP), P(TP), P(TP, None),
        P(EP, TP, None, None), P(EP), P(), P(), P(TP, EP), P(TP, EP), P(EP, TP),
        P(EP, None), P(EP, None), P(EP, None, TP), P(EP, None, TP), P(EP, TP, None),
    )
    out_specs = (P(EP, TP), P(EP, TP, None, None))
    return jax.shard_map(
        per_device, mesh=inner, in_specs=in_specs, out_specs=out_specs, check_vma=False
    )
```

```python
import jax
import jax.numpy as jnp
from jax import lax
from jax.experimental import pallas as pl
from jax.experimental.pallas import tpu as pltpu
from jax.sharding import Mesh, PartitionSpec as P

EPSILON = 1e-06
THETA = 10000.0
EP = ("z", "x")
TP = ("y", "c")
BF = jnp.bfloat16
F32 = jnp.float32
VMEM = pl.BlockSpec(memory_space=pltpu.VMEM)
HBM = pl.BlockSpec(memory_space=pltpu.HBM)


def exchange(value, axis):
    return lax.all_to_all(value, axis, split_axis=0, concat_axis=0, tiled=True)


def swap_cores(value):
    return lax.ppermute(value, "c", [(0, 1), (1, 0)])


def dot(a, b):
    return jnp.dot(a, b, preferred_element_type=F32)


def dot_nt(a, b):
    return lax.dot_general(a, b, (((1,), (1,)), ((), ())), preferred_element_type=F32)


def dot_tn(a, b):
    return lax.dot_general(a, b, (((0,), (0,)), ((), ())), preferred_element_type=F32)


def silu(x):
    return x * jax.nn.sigmoid(x)


def iota(shape, dim):
    return lax.broadcasted_iota(jnp.int32, shape, dim)


def call(body, name, out_shape, in_specs, scratch=(), limit=16):
    many = isinstance(out_shape, (list, tuple))
    return pl.pallas_call(
        body, name=name, out_shape=out_shape, in_specs=in_specs,
        out_specs=[VMEM] * len(out_shape) if many else VMEM,
        scratch_shapes=list(scratch),
        compiler_params=pltpu.CompilerParams(vmem_limit_bytes=limit * 1024 * 1024),
    )


def place_of():
    core = lax.axis_index("c")
    return core, lax.axis_index("y") * lax.axis_size("c") + core


def head_body(
    inverse, resid, gain, places, head_gain, wq, wk, wv, wg, wo, state,
    partial, key_out, value_out,
    r_mem, gain_mem, p_mem, hg_mem, q_mem, k_mem, v_mem, g_mem, o_mem, state_mem, carried_mem, sems,
):
    pairs = [
        (resid, r_mem), (gain, gain_mem), (places, p_mem), (head_gain, hg_mem),
        (wq, q_mem), (wk, k_mem), (state, state_mem), (wv, v_mem), (wg, g_mem), (wo, o_mem),
    ]
    moves = [pltpu.make_async_copy(src, dst, sems.at[i]) for i, (src, dst) in enumerate(pairs)]
    for move in moves:
        move.start()
    seqs, width = r_mem.shape
    size = q_mem.shape[1]
    _, tp = place_of()
    for move in moves[:4]:
        move.wait()
    x = r_mem[...].astype(F32)
    square = jnp.mean(x * x, axis=-1, keepdims=True)
    x = x * lax.rsqrt(square + EPSILON)
    gains = gain_mem[...].astype(F32)
    lanes = gains.shape[1]
    normed = jnp.concatenate(
        [
            (x[:, b * lanes : (b + 1) * lanes] * gains[b : b + 1, :]).astype(BF)
            for b in range(width // lanes)
        ],
        axis=1,
    )
    row = jnp.broadcast_to(p_mem[...].astype(F32), (seqs, seqs))
    eye = iota((seqs, seqs), 0) == iota((seqs, seqs), 1)
    column = jnp.sum(jnp.where(eye, row, 0.0), axis=1, keepdims=True)
    angles = column * inverse[...]
    cosine = jnp.cos(angles)
    sine = jnp.where(iota((seqs, size), 1) < size // 2, -1.0, 1.0) * jnp.sin(angles)

    def rotate(value):
        return value * cosine + pltpu.roll(value, size // 2, 1) * sine

    def project(move, mem):
        move.wait()
        return dot(normed, mem[...]).astype(BF).astype(F32)

    query = rotate(project(moves[4], q_mem))
    key = rotate(project(moves[5], k_mem)) * size ** (-0.5)
    key_out[...] = key
    turned = query.T
    moves[6].wait()
    for s in range(seqs):
        carried_mem[s : s + 1, :] = jnp.sum(
            state_mem[s] * turned[:, s : s + 1], axis=0, keepdims=True
        )
    value = project(moves[7], v_mem)
    value_out[...] = value
    head = jnp.full((seqs, size), tp, jnp.int32).astype(F32)
    decay = 1.0 - jnp.exp2(-1.0 - 1.5 * head)
    mixture = jnp.sum(query * key, axis=-1, keepdims=True) * value + decay * carried_mem[...]
    centre = jnp.mean(mixture, axis=-1, keepdims=True)
    moved = mixture - centre
    spread = jnp.mean(moved * moved, axis=-1, keepdims=True)
    normed_head = moved * lax.rsqrt(spread + EPSILON) * hg_mem[...].astype(F32)
    retained = (silu(project(moves[8], g_mem)) * normed_head).astype(BF)
    moves[9].wait()
    cols = partial.shape[2]
    for i in range(partial.shape[0]):
        partial[i] = dot(retained, o_mem[:, i * cols : (i + 1) * cols]).astype(BF)


def middle_body(arrived, resid, expert_pick, outgoing, middle_out):
    _, tp = place_of()
    groups, seqs, cols = arrived.shape
    total = resid[:, pl.ds(pl.multiple_of(tp * cols, cols), cols)].astype(F32)
    for i in range(groups):
        total = total + arrived[i].astype(F32)
    middle_out[...] = total
    cut = total.astype(BF)
    n_ep, rows, lanes = outgoing.shape
    pieces = cols // lanes
    n_x = lax.axis_size("x")
    share = seqs // n_x
    shape = (n_ep * share, seqs)
    to = iota(shape, 0)
    dense_pick = iota(shape, 1) == to // share % n_x * share + to % share
    dense_pick = dense_pick.astype(F32).astype(BF)
    expert = 0.0
    for h in range(pieces):
        part = cut[:, h * lanes : (h + 1) * lanes]
        dense = dot(dense_pick, part).astype(BF)
        outgoing[:, h * share : (h + 1) * share, :] = dense.reshape(n_ep, share, lanes)
        expert = expert + dot(expert_pick[h], part)
    outgoing[:, pieces * share :, :] = expert.astype(BF).reshape(n_ep, rows - pieces * share, lanes)


def dense_body(own, other, gains, mixers, *rest):
    out = rest[-1]
    n_x = lax.axis_size("x")
    weights, weights_other = rest[:n_x], rest[n_x : 2 * n_x]
    core, tp = place_of()
    x_index = lax.axis_index("x")
    sources, _, lanes = own.shape
    n_y = out.shape[0]
    hids, cols = weights[0].shape
    pieces = cols // lanes
    share = 32 // n_x
    slots = own.shape[1] // pieces - share
    n_slots = sources * slots
    half = sources // 2
    top = hids + 16
    shape = (pieces * n_slots, pieces * n_slots)
    to, at = iota(shape, 0), iota(shape, 1)
    row = to % n_slots
    turn = at == row // slots * (pieces * slots) + to // n_slots * slots + row % slots
    turn = turn.astype(F32).astype(BF)

    def expert_rows(ref, which):
        rows = ref[:, pieces * share :, :].reshape(pieces * n_slots, lanes)
        rows = dot(turn, rows).astype(BF)
        start = pl.multiple_of(top + which * pieces * n_slots, 16)
        for i in range(n_y):
            out[i, pl.ds(start, pieces * n_slots), :] = rows

    expert_rows(own, core)
    expert_rows(other, 1 - core)

    def columns(ref, which):
        table = ref[...].astype(F32)
        picked = [
            jnp.sum(jnp.where(iota(table.shape, 0) == which * pieces + h, table, 0.0),
                    axis=0, keepdims=True)
            for h in range(pieces)
        ]
        return jnp.concatenate(picked, axis=1)

    first = pl.multiple_of(core * half, half)

    def dense_rows(ref):
        return jnp.concatenate(
            [
                ref[pl.ds(first, half), h * share : (h + 1) * share, :]
                .reshape(half * share, lanes).astype(F32)
                for h in range(pieces)
            ],
            axis=1,
        )

    mine, theirs = dense_rows(own), dense_rows(other)
    x = (mine * columns(gains, tp)).astype(BF)
    x_other = (theirs * columns(gains, tp ^ 1)).astype(BF)
    ones = jnp.ones((16, cols), BF)
    squares = dot_nt(ones, (mine * mine).astype(BF)) + dot_nt(ones, (theirs * theirs).astype(BF))

    def mixer(which):
        return jnp.broadcast_to(columns(mixers, which), (16, cols)).astype(BF)

    mixes = dot_nt(mixer(tp), x) + dot_nt(mixer(tp ^ 1), x_other)
    low = jnp.where(iota(mixes.shape, 0) == 0, mixes, squares).astype(BF)
    for k in range(n_x):
        sums = dot_nt(weights[k][...], x) + dot_nt(weights_other[k][...], x_other)
        out[lax.rem(x_index + n_x - k, n_x), 0:hids, :] = sums.astype(BF)
    for i in range(n_y):
        out[i, hids:top, :] = low


def expert_body(
    got, gain, gate, up, down, hidden_out, send, keep, x_mem
):
    core, _ = place_of()
    n_y, _, lanes = got.shape
    hid = hidden_out.shape[0]
    n_slots, width = x_mem.shape
    top = 2 * hid + 16
    per_y = width // n_y // lanes
    square = jnp.zeros((n_slots, 1), F32)
    for b in range(width // lanes):
        start = top + b % per_y * n_slots
        piece = got[b // per_y, start : start + n_slots, :].astype(F32)
        square = square + jnp.sum(piece * piece, axis=1, keepdims=True)
    scale = lax.rsqrt(square / width + EPSILON)
    gains = gain[...].astype(F32)
    for b in range(width // lanes):
        start = top + b % per_y * n_slots
        piece = got[b // per_y, start : start + n_slots, :].astype(F32)
        part = slice(b * lanes, (b + 1) * lanes)
        x_mem[:, part] = (piece * scale * gains[b : b + 1, :]).astype(BF)

    sums = got[0, 0:top, :].astype(F32)
    for i in range(1, n_y):
        sums = sums + got[i, 0:top, :].astype(F32)
    factor = lax.rsqrt(sums[2 * hid + 1 : 2 * hid + 2] / width + EPSILON)
    mixing = jax.nn.sigmoid(sums[2 * hid : 2 * hid + 1] * factor)
    dense = silu(sums[:hid] * factor) * (sums[hid : 2 * hid] * factor) * mixing
    hidden_out[...] = dense.astype(BF)

    gates = dot(x_mem[...], gate[0])
    ups = dot(x_mem[...], up[0])
    hidden = (silu(gates) * ups).astype(BF)
    cols = width // n_y // 2
    for ref, which in ((send, 1 - core), (keep, core)):
        for i in range(n_y):
            start = pl.multiple_of(which * cols + i * 2 * cols, cols)
            ref[i] = dot(hidden, down[0, :, pl.ds(start, cols)]).astype(BF)


def pair_body(keep, got, hidden, hidden_other, out):
    core, _ = place_of()
    n_y, n_slots, cols = keep.shape
    lanes = out.shape[2]
    hid = hidden.shape[0]
    at = cols // lanes * n_slots
    for i in range(n_y):
        total = (keep[i].astype(F32) + got[i].astype(F32)).astype(BF)
        for h in range(cols // lanes):
            out[i, h * n_slots : (h + 1) * n_slots, :] = total[:, h * lanes : (h + 1) * lanes]
        out[i, pl.ds(pl.multiple_of(at + core * hid, 16), hid), :] = hidden[...]
        out[i, pl.ds(pl.multiple_of(at + (1 - core) * hid, 16), hid), :] = hidden_other[...]


def back_body(got, *rest):
    downs, out = rest[:-1], rest[-1]
    n_x = len(downs)
    x_index = lax.axis_index("x")
    n_y, _, lanes = got.shape
    hid, cols = downs[0].shape
    sources = out.shape[0]
    pieces = cols // lanes
    at = got.shape[1] - 2 * hid
    slots = at // pieces // sources
    share = out.shape[1] // pieces - slots
    result = got[0, 0:at, :].astype(F32)
    for i in range(1, n_y):
        result = result + got[i, 0:at, :].astype(F32)
    to = iota((at, at), 0)
    source, piece, slot = to // (pieces * slots), to // slots % pieces, to % slots
    turn = (iota((at, at), 1) == piece * (at // pieces) + source * slots + slot).astype(F32)
    result = dot(turn.astype(BF), result.astype(BF)).astype(BF)
    out[:, pieces * share :, :] = result.reshape(sources, pieces * slots, lanes)
    half = sources // 2
    for c in range(2):
        total = 0.0
        for k in range(n_x):
            hidden = got[lax.rem(x_index + n_x - k, n_x), at + c * hid : at + (c + 1) * hid, :]
            total = total + dot_tn(hidden, downs[k][...])
        total = total.astype(BF)
        for h in range(pieces):
            out[c * half : (c + 1) * half, h * share : (h + 1) * share, :] = total[
                :, h * lanes : (h + 1) * lanes
            ].reshape(half, share, lanes)


def final_body(back, weighing, middle, out):
    sources, _, lanes = back.shape
    seqs, cols = middle.shape
    pieces = cols // lanes
    n_x = lax.axis_size("x")
    share = seqs // n_x
    experts = back[:, pieces * share :, :].reshape(-1, lanes)
    for h in range(pieces):
        part = slice(h * lanes, (h + 1) * lanes)
        rows = slice(h * share, (h + 1) * share)
        dense = []
        for x in range(n_x):
            total = back[x, rows, :].astype(F32)
            for z in range(1, sources // n_x):
                total = total + back[z * n_x + x, rows, :].astype(F32)
            dense.append(total)
        total = jnp.concatenate(dense, axis=0) + dot(weighing[h], experts)
        out[:, part] = (middle[:, part] + total).astype(BF)


def per_device(
    resid, norm_gain, w_query, w_key, w_value, w_gate, head_gain, w_output, state, positions,
    ffn_gain, w_mix, dense_gate, dense_up, dense_down, routes, route_weight,
    expert_gate, expert_up, expert_down,
):
    sds = jax.ShapeDtypeStruct
    seqs, width = resid.shape
    n_y, n_c, n_x = lax.axis_size("y"), lax.axis_size("c"), lax.axis_size("x")
    n_tp = n_y * n_c
    n_ep = lax.axis_size("z") * n_x
    cols = width // n_tp
    tp = lax.axis_index("y") * n_c + lax.axis_index("c")
    slots = max(2, 2 * seqs * routes.shape[1] // n_ep)
    n_slots = n_ep * slots
    hid = dense_gate.shape[1]
    size = state.shape[2]
    lanes = 128
    pieces = cols // lanes
    share = seqs // n_x

    steps = jnp.arange(size, dtype=jnp.int32) % (size // 2)
    inverse = (THETA ** (-steps.astype(F32) / (size // 2)))[None, :]
    partial, key, value = call(
        head_body, "head",
        [sds((n_tp, seqs, cols), BF), sds((seqs, size), F32), sds((seqs, size), F32)],
        [VMEM] + [HBM] * 10,
        [pltpu.VMEM((seqs, width), BF), pltpu.VMEM((width // lanes, lanes), BF),
         pltpu.VMEM((1, seqs), jnp.int32), pltpu.VMEM((1, size), BF)]
        + [pltpu.VMEM((width, size), BF)] * 4
        + [pltpu.VMEM((size, width), BF), pltpu.VMEM((seqs, size, size), F32),
           pltpu.VMEM((seqs, size), F32), pltpu.SemaphoreType.DMA((10,))],
    )(inverse, *(pltpu.with_memory_space_constraint(w, pltpu.HBM) for w in (
        resid, norm_gain.reshape(width // lanes, lanes), positions[None], head_gain[None],
        w_query, w_key, w_value, w_gate, w_output, state.reshape(seqs, size, size))))
    decay = 1.0 - jnp.exp2(-1.0 - 1.5 * tp.astype(F32))
    new_state = decay * state + (key[:, :, None] * value[:, None, :])[:, None]
    partial, dense_gate, dense_up, dense_down = lax.optimization_barrier(
        (partial, dense_gate, dense_up, dense_down)
    )
    arrived = exchange(partial, TP)

    def from_x(value, k):
        return lax.ppermute(value, "x", [(i, (i + k) % n_x) for i in range(n_x)])

    both = jnp.concatenate([dense_gate.T, dense_up.T], axis=0)
    weights = [both] + [from_x(both, k) for k in range(1, n_x)]
    downs = [dense_down] + [from_x(dense_down, k) for k in range(1, n_x)]
    weights_other = [swap_cores(w) for w in weights]

    ids = jnp.arange(n_ep, dtype=jnp.int32)
    hits = routes[:, :, None] == ids
    named = jnp.any(hits, axis=1).astype(jnp.int32)
    before = jnp.cumsum(named, axis=0) - named
    slot_ids = jnp.arange(slots, dtype=jnp.int32)
    taken = (before[:, :, None] == slot_ids) & (named[:, :, None] == 1)
    which = jnp.arange(pieces)
    same = which[:, None, None, None, None] == which[None, None, None, :, None]
    taken = (taken[None, :, :, None, :] & same).reshape(pieces, seqs, pieces * n_slots)
    expert_pick = jnp.swapaxes(taken, 1, 2).astype(BF)
    weight_of = jnp.sum(jnp.where(hits, route_weight.astype(F32)[:, :, None], 0.0), axis=1)
    spread = jnp.repeat(weight_of, pieces * slots, axis=1)
    weighing = jnp.where(taken, spread[None], 0.0).astype(BF)

    outgoing, middle = call(
        middle_body, "middle",
        [sds((n_ep, pieces * (share + slots), lanes), BF), sds((seqs, cols), F32)], [VMEM] * 3,
    )(arrived, resid, expert_pick)
    rows = exchange(outgoing, EP)

    def table(value):
        return value.reshape(width // lanes, lanes)

    sent = call(
        dense_body, "dense", sds((n_y, 2 * hid + 16 + n_c * pieces * n_slots, lanes), BF),
        [VMEM] * (4 + 2 * n_x),
    )(rows, swap_cores(rows), table(ffn_gain), table(w_mix), *weights, *weights_other)
    got = exchange(sent, "y")

    hidden, send, keep = call(
        expert_body, "expert",
        [sds((hid, lanes), BF), sds((n_y, n_slots, cols), BF), sds((n_y, n_slots, cols), BF)],
        [VMEM] * 5,
        [pltpu.VMEM((n_slots, width), BF)],
    )(got, table(ffn_gain), expert_gate, expert_up, expert_down)
    sent = call(
        pair_body, "pair", sds((n_y, pieces * n_slots + n_c * hid, lanes), BF), [VMEM] * 4,
    )(keep, swap_cores(send), hidden, swap_cores(hidden))
    got = exchange(sent, "y")

    back = call(
        back_body, "back", sds((n_ep, pieces * (share + slots), lanes), BF), [VMEM] * (1 + n_x),
    )(got, *downs)
    back = exchange(back, EP)

    final = call(final_body, "final", sds((seqs, cols), BF), [VMEM] * 3)(back, weighing, middle)
    return (final, new_state)


def solution(mesh):
    inner = Mesh(mesh.devices.reshape(8, 4, 4, 2), ("z", "x", "y", "c"))
    in_specs = (
        P(EP, None), P(), P(None, TP), P(None, TP), P(None, TP), P(None, TP), P(TP), P(TP, None),
        P(EP, TP, None, None), P(EP), P(), P(), P(TP, EP), P(TP, EP), P(EP, TP),
        P(EP, None), P(EP, None), P(EP, None, TP), P(EP, None, TP), P(EP, TP, None),
    )
    out_specs = (P(EP, TP), P(EP, TP, None, None))
    return jax.shard_map(
        per_device, mesh=inner, in_specs=in_specs, out_specs=out_specs, check_vma=False
    )
```

```python
import functools

import jax
import jax.numpy as jnp
from jax import lax
from jax.experimental import pallas as pl
from jax.experimental.pallas import tpu as pltpu
from jax.sharding import Mesh, PartitionSpec as P


EPSILON = 1e-06
THETA = 10000.0
EP = ("z", "x")
TP = ("y", "c")
BF = jnp.bfloat16
F32 = jnp.float32
VMEM = pl.BlockSpec(memory_space=pltpu.VMEM)
HBM = pl.BlockSpec(memory_space=pltpu.HBM)


def exchange(value, axis):
    return lax.all_to_all(value, axis, split_axis=0, concat_axis=0, tiled=True)


def swap_cores(value):
    return lax.ppermute(value, "c", [(0, 1), (1, 0)])


def dot(a, b):
    return jnp.dot(a, b, preferred_element_type=F32)


def dot_nt(a, b):
    return lax.dot_general(a, b, (((1,), (1,)), ((), ())), preferred_element_type=F32)


def dot_tn(a, b):
    return lax.dot_general(a, b, (((0,), (0,)), ((), ())), preferred_element_type=F32)


def silu(x):
    return x * jax.nn.sigmoid(x)


def iota(shape, dim):
    return lax.broadcasted_iota(jnp.int32, shape, dim)


def call(body, out_shape, in_specs, scratch=(), limit=16):
    many = isinstance(out_shape, (list, tuple))
    return pl.pallas_call(
        body, out_shape=out_shape, in_specs=in_specs,
        out_specs=[VMEM] * len(out_shape) if many else VMEM,
        scratch_shapes=list(scratch),
        compiler_params=pltpu.CompilerParams(vmem_limit_bytes=limit * 1024 * 1024),
    )


def place_of():
    core = lax.axis_index("c")
    return core, lax.axis_index("y") * lax.axis_size("c") + core


def head_body(
    inverse, resid, gain, places, head_gain, wq, wk, wv, wg, wo, state,
    partial, key_out, value_out,
    r_mem, gain_mem, p_mem, hg_mem, q_mem, k_mem, v_mem, g_mem, o_mem, state_mem, carried_mem, sems,
):
    pairs = [
        (resid, r_mem), (gain, gain_mem), (places, p_mem), (head_gain, hg_mem),
        (wq, q_mem), (wk, k_mem), (state, state_mem), (wv, v_mem), (wg, g_mem), (wo, o_mem),
    ]
    moves = [pltpu.make_async_copy(src, dst, sems.at[i]) for i, (src, dst) in enumerate(pairs)]
    for move in moves:
        move.start()
    seqs, width = r_mem.shape
    size = q_mem.shape[1]
    _, tp = place_of()
    for move in moves[:4]:
        move.wait()
    x = r_mem[...].astype(F32)
    square = jnp.mean(x * x, axis=-1, keepdims=True)
    x = x * lax.rsqrt(square + EPSILON)
    gains = gain_mem[...].astype(F32)
    lanes = gains.shape[1]
    normed = jnp.concatenate(
        [
            (x[:, b * lanes : (b + 1) * lanes] * gains[b : b + 1, :]).astype(BF)
            for b in range(width // lanes)
        ],
        axis=1,
    )
    row = jnp.broadcast_to(p_mem[...].astype(F32), (seqs, seqs))
    eye = iota((seqs, seqs), 0) == iota((seqs, seqs), 1)
    column = jnp.sum(jnp.where(eye, row, 0.0), axis=1, keepdims=True)
    angles = column * inverse[...]
    cosine = jnp.cos(angles)
    sine = jnp.where(iota((seqs, size), 1) < size // 2, -1.0, 1.0) * jnp.sin(angles)

    def rotate(value):
        return value * cosine + pltpu.roll(value, size // 2, 1) * sine

    def project(move, mem):
        move.wait()
        return dot(normed, mem[...]).astype(BF).astype(F32)

    query = rotate(project(moves[4], q_mem))
    key = rotate(project(moves[5], k_mem)) * size ** (-0.5)
    key_out[...] = key
    turned = query.T
    moves[6].wait()
    for s in range(seqs):
        carried_mem[s : s + 1, :] = jnp.sum(
            state_mem[s] * turned[:, s : s + 1], axis=0, keepdims=True
        )
    value = project(moves[7], v_mem)
    value_out[...] = value
    head = jnp.full((seqs, size), tp, jnp.int32).astype(F32)
    decay = 1.0 - jnp.exp2(-1.0 - 1.5 * head)
    mixture = jnp.sum(query * key, axis=-1, keepdims=True) * value + decay * carried_mem[...]
    centre = jnp.mean(mixture, axis=-1, keepdims=True)
    moved = mixture - centre
    spread = jnp.mean(moved * moved, axis=-1, keepdims=True)
    normed_head = moved * lax.rsqrt(spread + EPSILON) * hg_mem[...].astype(F32)
    retained = (silu(project(moves[8], g_mem)) * normed_head).astype(BF)
    moves[9].wait()
    cols = partial.shape[2]
    for i in range(partial.shape[0]):
        partial[i] = dot(retained, o_mem[:, i * cols : (i + 1) * cols]).astype(BF)


def middle_body(arrived, resid, routes, weights, outgoing, middle_out, weighing):
    _, tp = place_of()
    groups, seqs, cols = arrived.shape
    n_ep, rows, lanes = outgoing.shape
    pieces = cols // lanes
    n_x = lax.axis_size("x")
    share = seqs // n_x
    per = rows - pieces * share
    slots = per // pieces

    def mask(value):
        return value.astype(F32).astype(BF)

    expert = iota((n_ep, seqs), 0)
    named = [expert == routes[j : j + 1, :] for j in range(routes.shape[0])]
    weight_of, hit = 0.0, 0.0
    for j, here in enumerate(named):
        hit = hit + here.astype(F32)
        weight_of = weight_of + jnp.where(here, weights[j : j + 1, :].astype(F32), 0.0)
    earlier = mask(iota((seqs, seqs), 0) < iota((seqs, seqs), 1))
    rank = jnp.where(hit > 0.5, dot(hit.astype(BF), earlier), 2.0 * seqs).astype(BF)
    shape = (n_ep * per, seqs)
    to = iota(shape, 0)
    repeat = mask(iota((n_ep * per, n_ep), 0) // per == iota((n_ep * per, n_ep), 1))
    taken = dot(repeat, rank) == (to % slots).astype(F32)
    weight_of = dot(repeat, weight_of.astype(BF))
    picks = []
    for h in range(pieces):
        here = taken & (to // slots % pieces == h)
        picks.append(mask(here))
        weighing[h] = jnp.where(here, weight_of, 0.0).astype(BF)
    shape = (n_ep * share, seqs)
    to = iota(shape, 0)
    dense_pick = mask(iota(shape, 1) == to // share % n_x * share + to % share)

    total = resid[:, pl.ds(pl.multiple_of(tp * cols, cols), cols)].astype(F32)
    for i in range(groups):
        total = total + arrived[i].astype(F32)
    middle_out[...] = total
    cut = total.astype(BF)
    chosen = 0.0
    for h in range(pieces):
        part = cut[:, h * lanes : (h + 1) * lanes]
        dense = dot(dense_pick, part).astype(BF)
        outgoing[:, h * share : (h + 1) * share, :] = dense.reshape(n_ep, share, lanes)
        chosen = chosen + dot(picks[h], part)
    outgoing[:, pieces * share :, :] = chosen.astype(BF).reshape(n_ep, per, lanes)


def dense_body(own, other, gains, mixers, *rest):
    out = rest[-1]
    n_x = lax.axis_size("x")
    n_blocks = len(rest) // 2
    weights, weights_other = rest[:n_blocks], rest[n_blocks : 2 * n_blocks]
    core, tp = place_of()
    sources, _, lanes = own.shape
    n_y = out.shape[0]
    hids, cols = weights[0].shape
    pieces = cols // lanes
    share = 32 // n_x
    slots = own.shape[1] // pieces - share
    n_slots = sources * slots
    top = hids + 16
    shape = (pieces * n_slots, pieces * n_slots)
    to, at = iota(shape, 0), iota(shape, 1)
    row = to % n_slots
    turn = at == row // slots * (pieces * slots) + to // n_slots * slots + row % slots
    turn = turn.astype(F32).astype(BF)

    def expert_rows(ref, which):
        rows = ref[:, pieces * share :, :].reshape(pieces * n_slots, lanes)
        rows = dot(turn, rows).astype(BF)
        start = pl.multiple_of(top + which * pieces * n_slots, 16)
        for i in range(n_y):
            out[i, pl.ds(start, pieces * n_slots), :] = rows

    expert_rows(own, core)
    expert_rows(other, 1 - core)

    def columns(ref, which):
        table = ref[...].astype(F32)
        picked = [
            jnp.sum(jnp.where(iota(table.shape, 0) == which * pieces + h, table, 0.0),
                    axis=0, keepdims=True)
            for h in range(pieces)
        ]
        return jnp.concatenate(picked, axis=1)

    def dense_rows(ref):
        return jnp.concatenate(
            [
                ref[:, h * share : (h + 1) * share, :].reshape(sources * share, lanes).astype(F32)
                for h in range(pieces)
            ],
            axis=1,
        )

    mine, theirs = dense_rows(own), dense_rows(other)
    x = (mine * columns(gains, tp)).astype(BF)
    x_other = (theirs * columns(gains, tp ^ 1)).astype(BF)
    ones = jnp.ones((16, cols), BF)
    squares = dot_nt(ones, (mine * mine).astype(BF)) + dot_nt(ones, (theirs * theirs).astype(BF))

    def mixer(which):
        return jnp.broadcast_to(columns(mixers, which), (16, cols)).astype(BF)

    mixes = dot_nt(mixer(tp), x) + dot_nt(mixer(tp ^ 1), x_other)
    low = jnp.where(iota(mixes.shape, 0) == 0, mixes, squares).astype(BF)
    halves = n_y // n_blocks
    for k in range(n_blocks):
        sums = (dot_nt(weights[k][...], x) + dot_nt(weights_other[k][...], x_other)).astype(BF)
        for t in range(halves):
            part = slice(t * lanes, (t + 1) * lanes)
            out[k * halves + t, 0:hids, :] = sums[:, part]
            out[k * halves + t, hids:top, :] = low[:, part]


def expert_body(
    got, gain, gate, up, hidden_out, expert_out, x_mem
):
    n_y, _, lanes = got.shape
    hid = hidden_out.shape[0]
    n_slots, width = x_mem.shape
    top = 2 * hid + 16
    per_y = width // n_y // lanes
    square = jnp.zeros((n_slots, 1), F32)
    for b in range(width // lanes):
        start = top + b % per_y * n_slots
        piece = got[b // per_y, start : start + n_slots, :].astype(F32)
        square = square + jnp.sum(piece * piece, axis=1, keepdims=True)
    scale = lax.rsqrt(square / width + EPSILON)
    gains = gain[...].astype(F32)
    for b in range(width // lanes):
        start = top + b % per_y * n_slots
        piece = got[b // per_y, start : start + n_slots, :].astype(F32)
        part = slice(b * lanes, (b + 1) * lanes)
        x_mem[:, part] = (piece * scale * gains[b : b + 1, :]).astype(BF)

    sums = got[0, 0:top, :].astype(F32)
    for i in range(1, n_y):
        sums = sums + got[i, 0:top, :].astype(F32)
    factor = lax.rsqrt(sums[2 * hid + 1 : 2 * hid + 2] / width + EPSILON)
    mixing = jax.nn.sigmoid(sums[2 * hid : 2 * hid + 1] * factor)
    dense = silu(sums[:hid] * factor) * (sums[hid : 2 * hid] * factor) * mixing
    hidden_out[...] = dense.astype(BF)

    gates = dot(x_mem[...], gate[0])
    ups = dot(x_mem[...], up[0])
    expert_out[...] = (silu(gates) * ups).astype(BF)


def down_body(other, hidden, down, out):
    core, _ = place_of()
    which = core ^ other
    n_y, _, cols = out.shape
    for i in range(n_y):
        start = pl.multiple_of(which * cols + i * 2 * cols, cols)
        out[i] = dot(hidden[...], down[0, :, pl.ds(start, cols)]).astype(BF)


def pair_body(keep, got, hidden, hidden_other, out):
    core, _ = place_of()
    n_y, n_slots, cols = keep.shape
    lanes = out.shape[2]
    hid = hidden.shape[0]
    at = cols // lanes * n_slots
    for i in range(n_y):
        total = (keep[i].astype(F32) + got[i].astype(F32)).astype(BF)
        for h in range(cols // lanes):
            out[i, h * n_slots : (h + 1) * n_slots, :] = total[:, h * lanes : (h + 1) * lanes]
        out[i, pl.ds(pl.multiple_of(at + core * hid, 16), hid), :] = hidden[...]
        out[i, pl.ds(pl.multiple_of(at + (1 - core) * hid, 16), hid), :] = hidden_other[...]


def back_body(got, *rest):
    downs, out = rest[:-1], rest[-1]
    n_x = len(downs)
    n_y, _, lanes = got.shape
    hid, cols = downs[0].shape
    sources = out.shape[0]
    pieces = cols // lanes
    at = got.shape[1] - 2 * hid
    slots = at // pieces // sources
    share = out.shape[1] // pieces - slots
    result = got[0, 0:at, :].astype(F32)
    for i in range(1, n_y):
        result = result + got[i, 0:at, :].astype(F32)
    to = iota((at, at), 0)
    source, piece, slot = to // (pieces * slots), to // slots % pieces, to % slots
    turn = (iota((at, at), 1) == piece * (at // pieces) + source * slots + slot).astype(F32)
    result = dot(turn.astype(BF), result.astype(BF)).astype(BF)
    out[:, pieces * share :, :] = result.reshape(sources, pieces * slots, lanes)
    halves = sources * share // lanes
    blocks = n_y // halves
    half = sources // halves
    for t in range(halves):
        total = 0.0
        for k in range(n_x):
            c, i = k // blocks, k % blocks * halves + t
            total = total + dot_tn(got[i, at + c * hid : at + (c + 1) * hid, :], downs[k][...])
        total = total.astype(BF)
        for h in range(pieces):
            out[t * half : (t + 1) * half, h * share : (h + 1) * share, :] = total[
                :, h * lanes : (h + 1) * lanes
            ].reshape(half, share, lanes)


def final_body(back, weighing, middle, out):
    sources, _, lanes = back.shape
    seqs, cols = middle.shape
    pieces = cols // lanes
    n_x = lax.axis_size("x")
    share = seqs // n_x
    experts = back[:, pieces * share :, :].reshape(-1, lanes)
    for h in range(pieces):
        part = slice(h * lanes, (h + 1) * lanes)
        rows = slice(h * share, (h + 1) * share)
        dense = []
        for x in range(n_x):
            total = back[x, rows, :].astype(F32)
            for z in range(1, sources // n_x):
                total = total + back[z * n_x + x, rows, :].astype(F32)
            dense.append(total)
        total = jnp.concatenate(dense, axis=0) + dot_tn(weighing[h], experts)
        out[:, part] = (middle[:, part] + total).astype(BF)


def one_device(
    resid, norm_gain, w_query, w_key, w_value, w_gate, head_gain, w_output, state, positions,
    ffn_gain, w_mix, dense_gate, dense_up, dense_down, routes, route_weight,
    expert_gate, expert_up, expert_down,
):
    sds = jax.ShapeDtypeStruct
    seqs, width = resid.shape
    n_y, n_c, n_x = lax.axis_size("y"), lax.axis_size("c"), lax.axis_size("x")
    n_tp = n_y * n_c
    n_ep = lax.axis_size("z") * n_x
    cols = width // n_tp
    tp = lax.axis_index("y") * n_c + lax.axis_index("c")
    slots = max(2, 2 * seqs * routes.shape[1] // n_ep)
    n_slots = n_ep * slots
    hid = dense_gate.shape[1]
    size = state.shape[2]
    lanes = 128
    pieces = cols // lanes
    share = seqs // n_x

    steps = jnp.arange(size, dtype=jnp.int32) % (size // 2)
    inverse = (THETA ** (-steps.astype(F32) / (size // 2)))[None, :]
    partial, key, value = call(
        head_body,
        [sds((n_tp, seqs, cols), BF), sds((seqs, size), F32), sds((seqs, size), F32)],
        [VMEM] + [HBM] * 10,
        [pltpu.VMEM((seqs, width), BF), pltpu.VMEM((width // lanes, lanes), BF),
         pltpu.VMEM((1, seqs), jnp.int32), pltpu.VMEM((1, size), BF)]
        + [pltpu.VMEM((width, size), BF)] * 4
        + [pltpu.VMEM((size, width), BF), pltpu.VMEM((seqs, size, size), F32),
           pltpu.VMEM((seqs, size), F32), pltpu.SemaphoreType.DMA((10,))],
    )(inverse, *(pltpu.with_memory_space_constraint(w, pltpu.HBM) for w in (
        resid, norm_gain.reshape(width // lanes, lanes), positions[None], head_gain[None],
        w_query, w_key, w_value, w_gate, w_output, state.reshape(seqs, size, size))))
    decay = 1.0 - jnp.exp2(-1.0 - 1.5 * tp.astype(F32))
    new_state = decay * state + (key[:, :, None] * value[:, None, :])[:, None]
    arrived = exchange(partial, TP)

    blocks = n_x // n_c
    both = jnp.concatenate([dense_gate.T, dense_up.T], axis=0)

    def piece(block, other):
        pairs = []
        for x in range(n_x):
            for c in range(n_c):
                source = (x + blocks * c + block) % n_x * n_c + (c ^ other)
                pairs.append((source, x * n_c + c))
        return lax.ppermute(both, ("x", "c"), pairs)

    weights = [piece(k, 0) for k in range(blocks)]
    weights_other = [piece(k, 1) for k in range(blocks)]
    downs = [dense_down] + [
        lax.ppermute(dense_down, "x", [((i + k) % n_x, i) for i in range(n_x)])
        for k in range(1, n_x)
    ]

    outgoing, middle, weighing = call(
        middle_body,
        [sds((n_ep, pieces * (share + slots), lanes), BF), sds((seqs, cols), F32),
         sds((pieces, pieces * n_slots, seqs), BF)],
        [VMEM] * 4,
    )(arrived, resid, routes.T, route_weight.T)
    rows = exchange(outgoing, EP)

    def table(value):
        return value.reshape(width // lanes, lanes)

    rows_other = swap_cores(rows)
    sent = call(
        dense_body, sds((n_y, 2 * hid + 16 + n_c * pieces * n_slots, lanes), BF),
        [VMEM] * (4 + 2 * blocks),
    )(rows, rows_other, table(ffn_gain), table(w_mix), *weights, *weights_other)
    got = exchange(sent, "y")

    hidden, expert_hidden = call(
        expert_body,
        [sds((hid, lanes), BF), sds((n_slots, expert_gate.shape[2]), BF)],
        [VMEM] * 4,
        [pltpu.VMEM((n_slots, width), BF)],
    )(got, table(ffn_gain), expert_gate, expert_up)

    def down_half(other):
        return call(
            functools.partial(down_body, other),
            sds((n_y, n_slots, cols), BF), [VMEM] * 2,
        )(expert_hidden, expert_down)

    send = down_half(1)
    half = swap_cores(send)
    keep = down_half(0)
    sent = call(
        pair_body, sds((n_y, pieces * n_slots + n_c * hid, lanes), BF), [VMEM] * 4,
    )(keep, half, hidden, swap_cores(hidden))
    got = exchange(sent, "y")

    back = call(
        back_body, sds((n_ep, pieces * (share + slots), lanes), BF),
        [VMEM] * (1 + n_x),
    )(got, *downs)
    back = exchange(back, EP)

    final = call(final_body, sds((seqs, cols), BF), [VMEM] * 3)(back, weighing, middle)
    return (final, new_state)


def solution(mesh):
    inner = Mesh(mesh.devices.reshape(8, 4, 4, 2), ("z", "x", "y", "c"))
    in_specs = (
        P(EP, None), P(), P(None, TP), P(None, TP), P(None, TP), P(None, TP), P(TP), P(TP, None),
        P(EP, TP, None, None), P(EP), P(), P(), P(TP, EP), P(TP, EP), P(EP, TP),
        P(EP, None), P(EP, None), P(EP, None, TP), P(EP, None, TP), P(EP, TP, None),
    )
    out_specs = (P(EP, TP), P(EP, TP, None, None))
    return jax.shard_map(
        one_device, mesh=inner, in_specs=in_specs, out_specs=out_specs, check_vma=False
    )
```

```python
import functools

import jax
import jax.numpy as jnp
from jax import lax
from jax.experimental import pallas as pl
from jax.experimental.pallas import tpu as pltpu
from jax.sharding import Mesh, PartitionSpec as P


EPSILON = 1e-06
THETA = 10000.0
EP = ("z", "x")
TP = ("y", "c")
BF = jnp.bfloat16
F32 = jnp.float32
VMEM = pl.BlockSpec(memory_space=pltpu.VMEM)
HBM = pl.BlockSpec(memory_space=pltpu.HBM)


def exchange(value, axis):
    return lax.all_to_all(value, axis, split_axis=0, concat_axis=0, tiled=True)


def swap_cores(value):
    return lax.ppermute(value, "c", [(0, 1), (1, 0)])


def dot(a, b):
    return jnp.dot(a, b, preferred_element_type=F32)


def dot_nt(a, b):
    return lax.dot_general(a, b, (((1,), (1,)), ((), ())), preferred_element_type=F32)


def dot_tn(a, b):
    return lax.dot_general(a, b, (((0,), (0,)), ((), ())), preferred_element_type=F32)


def silu(x):
    return x * jax.nn.sigmoid(x)


def iota(shape, dim):
    return lax.broadcasted_iota(jnp.int32, shape, dim)


def call(body, out_shape, in_specs, scratch=(), limit=16):
    many = isinstance(out_shape, (list, tuple))
    return pl.pallas_call(
        body, out_shape=out_shape, in_specs=in_specs,
        out_specs=[VMEM] * len(out_shape) if many else VMEM,
        scratch_shapes=list(scratch),
        compiler_params=pltpu.CompilerParams(vmem_limit_bytes=limit * 1024 * 1024),
    )


def place_of():
    core = lax.axis_index("c")
    return core, lax.axis_index("y") * lax.axis_size("c") + core


def head_body(
    inverse, resid, gain, places, head_gain, wq, wk, wv, wg, wo, state,
    partial, key_out, value_out,
    r_mem, gain_mem, p_mem, hg_mem, q_mem, k_mem, v_mem, g_mem, o_mem, state_mem, carried_mem, sems,
):
    pairs = [
        (resid, r_mem), (gain, gain_mem), (places, p_mem), (head_gain, hg_mem),
        (wq, q_mem), (wk, k_mem), (state, state_mem), (wv, v_mem), (wg, g_mem), (wo, o_mem),
    ]
    moves = [pltpu.make_async_copy(src, dst, sems.at[i]) for i, (src, dst) in enumerate(pairs)]
    for move in moves:
        move.start()
    seqs, width = r_mem.shape
    size = q_mem.shape[1]
    _, tp = place_of()
    for move in moves[:4]:
        move.wait()
    x = r_mem[...].astype(F32)
    square = jnp.mean(x * x, axis=-1, keepdims=True)
    x = x * lax.rsqrt(square + EPSILON)
    gains = gain_mem[...].astype(F32)
    lanes = gains.shape[1]
    normed = jnp.concatenate(
        [
            (x[:, b * lanes : (b + 1) * lanes] * gains[b : b + 1, :]).astype(BF)
            for b in range(width // lanes)
        ],
        axis=1,
    )
    row = jnp.broadcast_to(p_mem[...].astype(F32), (seqs, seqs))
    eye = iota((seqs, seqs), 0) == iota((seqs, seqs), 1)
    column = jnp.sum(jnp.where(eye, row, 0.0), axis=1, keepdims=True)
    angles = column * inverse[...]
    cosine = jnp.cos(angles)
    sine = jnp.where(iota((seqs, size), 1) < size // 2, -1.0, 1.0) * jnp.sin(angles)

    def rotate(value):
        return value * cosine + pltpu.roll(value, size // 2, 1) * sine

    def project(move, mem):
        move.wait()
        return dot(normed, mem[...]).astype(BF).astype(F32)

    query = rotate(project(moves[4], q_mem))
    key = rotate(project(moves[5], k_mem)) * size ** (-0.5)
    key_out[...] = key
    turned = query.T
    moves[6].wait()
    for s in range(seqs):
        carried_mem[s : s + 1, :] = jnp.sum(
            state_mem[s] * turned[:, s : s + 1], axis=0, keepdims=True
        )
    value = project(moves[7], v_mem)
    value_out[...] = value
    head = jnp.full((seqs, size), tp, jnp.int32).astype(F32)
    decay = 1.0 - jnp.exp2(-1.0 - 1.5 * head)
    mixture = jnp.sum(query * key, axis=-1, keepdims=True) * value + decay * carried_mem[...]
    centre = jnp.mean(mixture, axis=-1, keepdims=True)
    moved = mixture - centre
    spread = jnp.mean(moved * moved, axis=-1, keepdims=True)
    normed_head = moved * lax.rsqrt(spread + EPSILON) * hg_mem[...].astype(F32)
    retained = (silu(project(moves[8], g_mem)) * normed_head).astype(BF)
    moves[9].wait()
    cols = partial.shape[2]
    for i in range(partial.shape[0]):
        partial[i] = dot(retained, o_mem[:, i * cols : (i + 1) * cols]).astype(BF)


def middle_body(arrived, resid, routes, weights, outgoing, middle_out, weighing):
    _, tp = place_of()
    groups, seqs, cols = arrived.shape
    n_ep, rows, lanes = outgoing.shape
    pieces = cols // lanes
    n_x = lax.axis_size("x")
    share = seqs // n_x
    per = rows - pieces * share
    slots = per // pieces

    def mask(value):
        return value.astype(F32).astype(BF)

    expert = iota((n_ep, seqs), 0)
    named = [expert == routes[j : j + 1, :] for j in range(routes.shape[0])]
    weight_of, hit = 0.0, 0.0
    for j, here in enumerate(named):
        hit = hit + here.astype(F32)
        weight_of = weight_of + jnp.where(here, weights[j : j + 1, :].astype(F32), 0.0)
    earlier = mask(iota((seqs, seqs), 0) < iota((seqs, seqs), 1))
    rank = jnp.where(hit > 0.5, dot(hit.astype(BF), earlier), 2.0 * seqs).astype(BF)
    shape = (n_ep * per, seqs)
    to = iota(shape, 0)
    repeat = mask(iota((n_ep * per, n_ep), 0) // per == iota((n_ep * per, n_ep), 1))
    taken = dot(repeat, rank) == (to % slots).astype(F32)
    weight_of = dot(repeat, weight_of.astype(BF))
    picks = []
    for h in range(pieces):
        here = taken & (to // slots % pieces == h)
        picks.append(mask(here))
        weighing[h] = jnp.where(here, weight_of, 0.0).astype(BF)
    shape = (n_ep * share, seqs)
    to = iota(shape, 0)
    dense_pick = mask(iota(shape, 1) == to // share % n_x * share + to % share)

    total = resid[:, pl.ds(pl.multiple_of(tp * cols, cols), cols)].astype(F32)
    for i in range(groups):
        total = total + arrived[i].astype(F32)
    middle_out[...] = total
    cut = total.astype(BF)
    chosen = 0.0
    for h in range(pieces):
        part = cut[:, h * lanes : (h + 1) * lanes]
        dense = dot(dense_pick, part).astype(BF)
        outgoing[:, h * share : (h + 1) * share, :] = dense.reshape(n_ep, share, lanes)
        chosen = chosen + dot(picks[h], part)
    outgoing[:, pieces * share :, :] = chosen.astype(BF).reshape(n_ep, per, lanes)


def dense_body(own, other, gains, mixers, *rest):
    out = rest[-1]
    n_x = lax.axis_size("x")
    n_blocks = len(rest) // 2
    weights, weights_other = rest[:n_blocks], rest[n_blocks : 2 * n_blocks]
    _, tp = place_of()
    sources, _, lanes = own.shape
    n_y = out.shape[0]
    hids, cols = weights[0].shape
    pieces = cols // lanes
    share = 32 // n_x
    slots = own.shape[1] // pieces - share
    n_slots = sources * slots
    top = hids + 16
    shape = (pieces * n_slots, pieces * n_slots)
    to, at = iota(shape, 0), iota(shape, 1)
    row = to % n_slots
    turn = at == row // slots * (pieces * slots) + to // n_slots * slots + row % slots
    turn = turn.astype(F32).astype(BF)

    rows = own[:, pieces * share :, :].reshape(pieces * n_slots, lanes)
    rows = dot(turn, rows).astype(BF)
    for i in range(n_y):
        out[i, top:, :] = rows

    def columns(ref, which):
        table = ref[...].astype(F32)
        picked = [
            jnp.sum(jnp.where(iota(table.shape, 0) == which * pieces + h, table, 0.0),
                    axis=0, keepdims=True)
            for h in range(pieces)
        ]
        return jnp.concatenate(picked, axis=1)

    def dense_rows(ref):
        return jnp.concatenate(
            [
                ref[:, h * share : (h + 1) * share, :].reshape(sources * share, lanes).astype(F32)
                for h in range(pieces)
            ],
            axis=1,
        )

    mine, theirs = dense_rows(own), dense_rows(other)
    x = (mine * columns(gains, tp)).astype(BF)
    x_other = (theirs * columns(gains, tp ^ 1)).astype(BF)
    ones = jnp.ones((16, cols), BF)
    squares = dot_nt(ones, (mine * mine).astype(BF)) + dot_nt(ones, (theirs * theirs).astype(BF))

    def mixer(which):
        return jnp.broadcast_to(columns(mixers, which), (16, cols)).astype(BF)

    mixes = dot_nt(mixer(tp), x) + dot_nt(mixer(tp ^ 1), x_other)
    low = jnp.where(iota(mixes.shape, 0) == 0, mixes, squares).astype(BF)
    halves = n_y // n_blocks
    for k in range(n_blocks):
        sums = (dot_nt(weights[k][...], x) + dot_nt(weights_other[k][...], x_other)).astype(BF)
        for t in range(halves):
            part = slice(t * lanes, (t + 1) * lanes)
            out[k * halves + t, 0:hids, :] = sums[:, part]
            out[k * halves + t, hids:top, :] = low[:, part]


def hidden_body(got, hidden_out, rows_out):
    n_y, _, lanes = got.shape
    hid = hidden_out.shape[0]
    top = 2 * hid + 16
    width = 2 * n_y * (rows_out.shape[1] // 128) * lanes
    sums = got[0, 0:top, :].astype(F32)
    for i in range(1, n_y):
        sums = sums + got[i, 0:top, :].astype(F32)
    for i in range(n_y):
        rows_out[i] = got[i, top:, :]
    factor = lax.rsqrt(sums[2 * hid + 1 : 2 * hid + 2] / width + EPSILON)
    mixing = jax.nn.sigmoid(sums[2 * hid : 2 * hid + 1] * factor)
    dense = silu(sums[:hid] * factor) * (sums[hid : 2 * hid] * factor) * mixing
    hidden_out[...] = dense.astype(BF)


def expert_body(mine, theirs, gain, gate, up, expert_out, x_mem):
    core, _ = place_of()
    n_y, _, lanes = mine.shape
    n_slots, width = x_mem.shape
    per_y = width // n_y // lanes
    pieces = per_y // 2
    square = jnp.zeros((n_slots, 1), F32)
    for i in range(n_y):
        for h in range(pieces):
            for ref in (mine, theirs):
                piece = ref[i, h * n_slots : (h + 1) * n_slots, :].astype(F32)
                square = square + jnp.sum(piece * piece, axis=1, keepdims=True)
    scale = lax.rsqrt(square / width + EPSILON)
    gains = gain[...].astype(F32)
    for i in range(n_y):
        for h in range(pieces):
            here = mine[i, h * n_slots : (h + 1) * n_slots, :].astype(F32)
            there = theirs[i, h * n_slots : (h + 1) * n_slots, :].astype(F32)
            for c in range(2):
                b = i * per_y + c * pieces + h
                piece = jnp.where(core == c, here, there) * scale * gains[b : b + 1, :]
                x_mem[:, b * lanes : (b + 1) * lanes] = piece.astype(BF)
    gates = dot(x_mem[...], gate[0])
    ups = dot(x_mem[...], up[0])
    expert_out[...] = (silu(gates) * ups).astype(BF)


def fetch_body(source, out, sems):
    moves = []
    for i in range(sems.shape[0]):
        step = source.shape[1] // sems.shape[0]
        part = pl.ds(i * step, step)
        moves.append(pltpu.make_async_copy(source.at[0, part], out.at[0, part], sems.at[i]))
        moves[-1].start()
    for move in moves:
        move.wait()


def down_body(other, hidden, down, out):
    core, _ = place_of()
    which = core ^ other
    n_y, _, cols = out.shape
    for i in range(n_y):
        start = pl.multiple_of(which * cols + i * 2 * cols, cols)
        out[i] = dot(hidden[...], down[0, :, pl.ds(start, cols)]).astype(BF)


def pair_body(keep, got, hidden, hidden_other, out):
    core, _ = place_of()
    n_y, n_slots, cols = keep.shape
    lanes = out.shape[2]
    hid = hidden.shape[0]
    at = cols // lanes * n_slots
    for i in range(n_y):
        total = (keep[i].astype(F32) + got[i].astype(F32)).astype(BF)
        for h in range(cols // lanes):
            out[i, h * n_slots : (h + 1) * n_slots, :] = total[:, h * lanes : (h + 1) * lanes]
        out[i, pl.ds(pl.multiple_of(at + core * hid, 16), hid), :] = hidden[...]
        out[i, pl.ds(pl.multiple_of(at + (1 - core) * hid, 16), hid), :] = hidden_other[...]


def back_body(got, *rest):
    downs, out = rest[:-1], rest[-1]
    n_x = len(downs)
    n_y, _, lanes = got.shape
    hid, cols = downs[0].shape
    sources = out.shape[0]
    pieces = cols // lanes
    at = got.shape[1] - 2 * hid
    slots = at // pieces // sources
    share = out.shape[1] // pieces - slots
    result = got[0, 0:at, :].astype(F32)
    for i in range(1, n_y):
        result = result + got[i, 0:at, :].astype(F32)
    to = iota((at, at), 0)
    source, piece, slot = to // (pieces * slots), to // slots % pieces, to % slots
    turn = (iota((at, at), 1) == piece * (at // pieces) + source * slots + slot).astype(F32)
    result = dot(turn.astype(BF), result.astype(BF)).astype(BF)
    out[:, pieces * share :, :] = result.reshape(sources, pieces * slots, lanes)
    halves = sources * share // lanes
    blocks = n_y // halves
    half = sources // halves
    for t in range(halves):
        total = 0.0
        for k in range(n_x):
            c, i = k // blocks, k % blocks * halves + t
            total = total + dot_tn(got[i, at + c * hid : at + (c + 1) * hid, :], downs[k][...])
        total = total.astype(BF)
        for h in range(pieces):
            out[t * half : (t + 1) * half, h * share : (h + 1) * share, :] = total[
                :, h * lanes : (h + 1) * lanes
            ].reshape(half, share, lanes)


def final_body(back, weighing, middle, out):
    sources, _, lanes = back.shape
    seqs, cols = middle.shape
    pieces = cols // lanes
    n_x = lax.axis_size("x")
    share = seqs // n_x
    experts = back[:, pieces * share :, :].reshape(-1, lanes)
    for h in range(pieces):
        part = slice(h * lanes, (h + 1) * lanes)
        rows = slice(h * share, (h + 1) * share)
        dense = []
        for x in range(n_x):
            total = back[x, rows, :].astype(F32)
            for z in range(1, sources // n_x):
                total = total + back[z * n_x + x, rows, :].astype(F32)
            dense.append(total)
        total = jnp.concatenate(dense, axis=0) + dot_tn(weighing[h], experts)
        out[:, part] = (middle[:, part] + total).astype(BF)


def one_device(
    resid, norm_gain, w_query, w_key, w_value, w_gate, head_gain, w_output, state, positions,
    ffn_gain, w_mix, dense_gate, dense_up, dense_down, routes, route_weight,
    expert_gate, expert_up, expert_down,
):
    sds = jax.ShapeDtypeStruct
    seqs, width = resid.shape
    n_y, n_c, n_x = lax.axis_size("y"), lax.axis_size("c"), lax.axis_size("x")
    n_tp = n_y * n_c
    n_ep = lax.axis_size("z") * n_x
    cols = width // n_tp
    tp = lax.axis_index("y") * n_c + lax.axis_index("c")
    slots = max(2, 2 * seqs * routes.shape[1] // n_ep)
    n_slots = n_ep * slots
    hid = dense_gate.shape[1]
    size = state.shape[2]
    lanes = 128
    pieces = cols // lanes
    share = seqs // n_x

    steps = jnp.arange(size, dtype=jnp.int32) % (size // 2)
    inverse = (THETA ** (-steps.astype(F32) / (size // 2)))[None, :]
    partial, key, value = call(
        head_body,
        [sds((n_tp, seqs, cols), BF), sds((seqs, size), F32), sds((seqs, size), F32)],
        [VMEM] + [HBM] * 10,
        [pltpu.VMEM((seqs, width), BF), pltpu.VMEM((width // lanes, lanes), BF),
         pltpu.VMEM((1, seqs), jnp.int32), pltpu.VMEM((1, size), BF)]
        + [pltpu.VMEM((width, size), BF)] * 4
        + [pltpu.VMEM((size, width), BF), pltpu.VMEM((seqs, size, size), F32),
           pltpu.VMEM((seqs, size), F32), pltpu.SemaphoreType.DMA((10,))],
    )(inverse, *(pltpu.with_memory_space_constraint(w, pltpu.HBM) for w in (
        resid, norm_gain.reshape(width // lanes, lanes), positions[None], head_gain[None],
        w_query, w_key, w_value, w_gate, w_output, state.reshape(seqs, size, size))))
    decay = 1.0 - jnp.exp2(-1.0 - 1.5 * tp.astype(F32))
    new_state = decay * state + (key[:, :, None] * value[:, None, :])[:, None]
    arrived = exchange(partial, TP)

    blocks = n_x // n_c
    both = jnp.concatenate([dense_gate.T, dense_up.T], axis=0)

    def piece(block, other):
        pairs = []
        for x in range(n_x):
            for c in range(n_c):
                source = (x + blocks * c + block) % n_x * n_c + (c ^ other)
                pairs.append((source, x * n_c + c))
        return lax.ppermute(both, ("x", "c"), pairs)

    weights = [piece(k, 0) for k in range(blocks)]
    weights_other = [piece(k, 1) for k in range(blocks)]
    downs = [dense_down] + [
        lax.ppermute(dense_down, "x", [((i + k) % n_x, i) for i in range(n_x)])
        for k in range(1, n_x)
    ]

    outgoing, middle, weighing = call(
        middle_body,
        [sds((n_ep, pieces * (share + slots), lanes), BF), sds((seqs, cols), F32),
         sds((pieces, pieces * n_slots, seqs), BF)],
        [VMEM] * 4,
    )(arrived, resid, routes.T, route_weight.T)
    rows = exchange(outgoing, EP)

    expert_up = call(
        fetch_body, sds(expert_up.shape, BF), [HBM],
        [pltpu.SemaphoreType.DMA((4,))],
    )(pltpu.with_memory_space_constraint(expert_up, pltpu.HBM))

    def table(value):
        return value.reshape(width // lanes, lanes)

    rows_other = swap_cores(rows)
    sent = call(
        dense_body, sds((n_y, 2 * hid + 16 + pieces * n_slots, lanes), BF),
        [VMEM] * (4 + 2 * blocks),
    )(rows, rows_other, table(ffn_gain), table(w_mix), *weights, *weights_other)
    got = exchange(sent, "y")

    hidden, expert_rows = call(
        hidden_body,
        [sds((hid, lanes), BF), sds((n_y, pieces * n_slots, lanes), BF)], [VMEM],
    )(got)
    rows_there = swap_cores(expert_rows)
    hidden_other = swap_cores(hidden)
    expert_hidden = call(
        expert_body, sds((n_slots, expert_gate.shape[2]), BF), [VMEM] * 5,
        [pltpu.VMEM((n_slots, width), BF)],
    )(expert_rows, rows_there, table(ffn_gain), expert_gate, expert_up)

    def down_half(other):
        return call(
            functools.partial(down_body, other),
            sds((n_y, n_slots, cols), BF), [VMEM] * 2,
        )(expert_hidden, expert_down)

    send = down_half(1)
    half = swap_cores(send)
    keep = down_half(0)
    sent = call(
        pair_body, sds((n_y, pieces * n_slots + n_c * hid, lanes), BF), [VMEM] * 4,
    )(keep, half, hidden, hidden_other)
    got = exchange(sent, "y")

    back = call(
        back_body, sds((n_ep, pieces * (share + slots), lanes), BF),
        [VMEM] * (1 + n_x),
    )(got, *downs)
    back = exchange(back, EP)

    final = call(final_body, sds((seqs, cols), BF), [VMEM] * 3)(back, weighing, middle)
    return (final, new_state)


def solution(mesh):
    inner = Mesh(mesh.devices.reshape(8, 4, 4, 2), ("z", "x", "y", "c"))
    in_specs = (
        P(EP, None), P(), P(None, TP), P(None, TP), P(None, TP), P(None, TP), P(TP), P(TP, None),
        P(EP, TP, None, None), P(EP), P(), P(), P(TP, EP), P(TP, EP), P(EP, TP),
        P(EP, None), P(EP, None), P(EP, None, TP), P(EP, None, TP), P(EP, TP, None),
    )
    out_specs = (P(EP, TP), P(EP, TP, None, None))
    return jax.shard_map(
        one_device, mesh=inner, in_specs=in_specs, out_specs=out_specs, check_vma=False
    )
```
